32 devices in a mesh: sp: 8 (over z, y), tp: 4 (over x, core).
Axes of the slice: x: 2, y: 2, z: 4, core: 2. Of those that a mesh axis runs over, the one named last changes fastest.
Arguments:
- tokens: bfloat16 [3072, 2048], P('sp', 'tp'), may hold values from -6 to 6
- norm_gain: float32 [2048], replicated, may hold values from 0.1 to 1.9
- w_query_down: bfloat16 [2048, 512], replicated, may hold values from -0.125 to 0.125
- query_gain: float32 [512], replicated, may hold values from 0.1 to 1.9
- w_query_up: bfloat16 [512, 1536], P(None, 'tp'), may hold values from -0.25 to 0.25
- w_latent_down: bfloat16 [2048, 256], replicated, may hold values from -0.125 to 0.125
- latent_gain: float32 [256], replicated, may hold values from 0.1 to 1.9
- w_rotary_key: bfloat16 [2048, 32], replicated, may hold values from -0.125 to 0.125
- w_latent_up: bfloat16 [256, 2048], P(None, 'tp'), may hold values from -0.375 to 0.375
- query_head_gain: float32 [96], replicated, may hold values from 0.1 to 1.9
- key_head_gain: float32 [96], replicated, may hold values from 0.1 to 1.9
- w_pool_in: bfloat16 [2048, 1024], P(None, 'tp'), may hold values from -0.125 to 0.125
- w_pool_mix: bfloat16 [4, 256, 256], P('tp'), may hold values from -0.375 to 0.375
- pool_scale: float32 [1024], P('tp'), may hold values from 0.1 to 1.9
- w_attn_out: bfloat16 [1024, 2048], P('tp'), may hold values from -12 to 12
- w_pool_out: bfloat16 [1024, 2048], P('tp'), may hold values from -0.5 to 0.5
- w_gate_attn: bfloat16 [2048, 2048], P(None, 'tp'), may hold values from -0.125 to 0.125
- w_gate_pool: bfloat16 [2048, 2048], P(None, 'tp'), may hold values from -0.125 to 0.125
Outputs:
- mixed: bfloat16 [3072, 2048], P('sp', 'tp')
The draws below stay inside these ranges and needn't reach their ends.
All inputs are finite; a program needn't handle non-finite values.
Results may differ from the reference program's by a relative error of at most 0.02.
Values may be sent and summed in bfloat16 or wider, within the bound.
A program may use at most 128 MiB of HBM per device.

```python
import math
import jax
import jax.numpy as jnp
from jax import lax

D = 2048
HEADS = 16
QUERY_RANK = 512
LATENT_RANK = 256
NOPE = 64
ROPE = 32
VALUE_DIM = 64
POOL_GROUPS = 4
POOL_GROUP = 256
POOL_WIDTH = 1024
TOKENS = 3072


def level_of(rng, extent, pieces, smallest, top_value):
    def one(dim, shards_of):
        steps = jax.random.uniform(jax.random.fold_in(jax.random.fold_in(rng, 6), dim), (shards_of,), jnp.float32, smallest / len(pieces), top_value / len(pieces))
        return jnp.repeat(jnp.exp(steps), extent[dim] // shards_of).reshape((-1,) + (1,) * (len(extent) - dim - 1))

    level = one(*pieces[0])
    for cut in pieces[1:]:
        level = level * one(*cut)
    return level


def centred(own_key, shape, deviation, most, split=(), held_as=jnp.bfloat16):
    result = jax.random.normal(own_key, shape, jnp.float32) * deviation
    if len(split) > 0:
        result = level_of(own_key, shape, split, -0.22, 0.18) * result
    return jnp.clip(result, min=-most, max=most).astype(held_as)


def setup_inputs(seed: int = 0) -> dict:
    streams_of = jax.random.split(jax.random.key(seed), 19)
    return {
        "tokens": centred(streams_of[0], (TOKENS, D), 1.0, 6.0, ((0, 8), (1, 4))),
        "norm_gain": jnp.clip(1.0 + 0.18 * jax.random.normal(streams_of[1], (D,), jnp.float32), 0.1, 1.9),
        "w_query_down": centred(streams_of[2], (D, QUERY_RANK), D ** -0.5, 0.125),
        "query_gain": jnp.clip(1.0 + 0.18 * jax.random.normal(streams_of[3], (QUERY_RANK,), jnp.float32), 0.1, 1.9),
        "w_query_up": centred(streams_of[4], (QUERY_RANK, HEADS * (NOPE + ROPE)), QUERY_RANK ** -0.5, 0.25, ((1, 4),)),
        "w_latent_down": centred(streams_of[5], (D, LATENT_RANK), D ** -0.5, 0.125),
        "latent_gain": jnp.clip(1.0 + 0.18 * jax.random.normal(streams_of[6], (LATENT_RANK,), jnp.float32), 0.1, 1.9),
        "w_rotary_key": centred(streams_of[7], (D, ROPE), D ** -0.5, 0.125),
        "w_latent_up": centred(streams_of[8], (LATENT_RANK, HEADS * (NOPE + VALUE_DIM)), LATENT_RANK ** -0.5, 0.375, ((1, 4),)),
        "query_head_gain": jnp.clip(1.0 + 0.18 * jax.random.normal(streams_of[9], (NOPE + ROPE,), jnp.float32), 0.1, 1.9),
        "key_head_gain": jnp.clip(1.0 + 0.18 * jax.random.normal(streams_of[10], (NOPE + ROPE,), jnp.float32), 0.1, 1.9),
        "w_pool_in": centred(streams_of[11], (D, POOL_WIDTH), D ** -0.5, 0.125, ((1, 4),)),
        "w_pool_mix": centred(streams_of[12], (POOL_GROUPS, POOL_GROUP, POOL_GROUP), POOL_GROUP ** -0.5, 0.375, ((0, 4),)),
        "pool_scale": jnp.clip(1.0 + 0.18 * jax.random.normal(streams_of[13], (POOL_WIDTH,), jnp.float32), 0.1, 1.9),
        "w_attn_out": centred(streams_of[14], (HEADS * VALUE_DIM, D), 2.0, 12.0, ((0, 4),)),
        "w_pool_out": centred(streams_of[15], (POOL_WIDTH, D), (POOL_WIDTH // 8) ** -0.5, 0.5, ((0, 4),)),
        "w_gate_attn": centred(streams_of[16], (D, D), D ** -0.5, 0.125, ((1, 4),)),
        "w_gate_pool": centred(streams_of[17], (D, D), D ** -0.5, 0.125, ((1, 4),)),
    }


eps = 1e-06
theta = 10000.0

def rms_scale(values, gain):
    values = values.astype(jnp.float32)
    return values * lax.rsqrt(lax.optimization_barrier(jnp.mean(values * values, axis=-1, keepdims=True)) + eps) * gain

def rotate(values, positions):
    half = values.shape[-1] // 2
    freqs = theta ** (-jnp.arange(half, dtype=jnp.float32) / half)
    angles = positions.astype(jnp.float32)[:, None] * freqs[None, :]
    cosine = jnp.cos(angles)[:, None, :]
    sine = jnp.sin(angles)[:, None, :]
    first = values[..., :half]
    second = values[..., half:]
    return jnp.concatenate([first * cosine - second * sine, first * sine + second * cosine], axis=-1)

def head_finish(values, gain, positions):
    normed = rms_scale(values, gain)
    return jnp.concatenate([normed[..., :NOPE], rotate(normed[..., NOPE:], positions)], axis=-1)

def reference(tokens, norm_gain, w_query_down, query_gain, w_query_up, w_latent_down, latent_gain, w_rotary_key, w_latent_up, query_head_gain, key_head_gain, w_pool_in, w_pool_mix, pool_scale, w_attn_out, w_pool_out, w_gate_attn, w_gate_pool):
    length = tokens.shape[0]
    bf = jnp.bfloat16
    positions = jnp.arange(length, dtype=jnp.int32)
    normed = rms_scale(tokens, norm_gain).astype(bf)
    query_latent = jnp.dot(normed, w_query_down, preferred_element_type=jnp.float32).astype(bf)
    query_normed = rms_scale(query_latent, query_gain).astype(bf)
    query_raw = jnp.dot(query_normed, w_query_up, preferred_element_type=jnp.float32).astype(bf)
    query_raw = query_raw.reshape(length, HEADS, NOPE + ROPE)
    query = (head_finish(query_raw, query_head_gain, positions) * (NOPE + ROPE) ** (-0.5)).astype(bf)
    latent = jnp.dot(normed, w_latent_down, preferred_element_type=jnp.float32).astype(bf)
    key_latent = rms_scale(latent, latent_gain).astype(bf)
    rotary_key = jnp.dot(normed, w_rotary_key, preferred_element_type=jnp.float32).astype(bf)
    keys_values = jnp.dot(key_latent, w_latent_up, preferred_element_type=jnp.float32).astype(bf)
    keys_values = keys_values.reshape(length, HEADS, NOPE + VALUE_DIM)
    key_raw = jnp.concatenate([keys_values[..., :NOPE], jnp.broadcast_to(rotary_key[:, None, :], (length, HEADS, ROPE))], axis=-1)
    key = head_finish(key_raw, key_head_gain, positions).astype(bf).astype(jnp.float32)
    values = keys_values[..., NOPE:].astype(jnp.float32)
    block = math.gcd(length, 256)
    query_blocks = query.reshape(length // block, block, HEADS, NOPE + ROPE)

    def attend(query_block):
        scores = jnp.einsum('qhd,khd->hqk', query_block.astype(jnp.float32), key)
        top = lax.optimization_barrier(jnp.max(scores, axis=-1, keepdims=True))
        expo = jnp.exp(scores - top)
        total = lax.optimization_barrier(jnp.sum(expo, axis=-1))
        rounded = lax.optimization_barrier(expo.astype(bf)).astype(jnp.float32)
        weighted = jnp.einsum('hqk,khv->qhv', rounded, values)
        return (weighted / jnp.transpose(total)[:, :, None]).astype(bf)
    attn_rows = lax.map(attend, query_blocks).reshape(length, HEADS * VALUE_DIM)
    pool_input = jnp.dot(normed, w_pool_in, preferred_element_type=jnp.float32).astype(bf)
    reach = 2 ** POOL_GROUPS // 2
    padded = jnp.pad(pool_input.astype(jnp.float32), ((reach, reach), (0, 0)))
    windows = jnp.power(2, jnp.arange(POOL_GROUPS, dtype=jnp.int32) + 1)
    channel_window = jnp.repeat(windows, POOL_GROUP)
    total = jnp.zeros((length, POOL_GROUPS * POOL_GROUP), jnp.float32)
    for shift in range(-reach, reach):
        inside = (shift >= -(channel_window // 2)) & (shift <= channel_window - channel_window // 2 - 1)
        total = total + jnp.where(inside[None, :], padded[reach + shift:reach + shift + length], 0.0)
    low = jnp.clip(positions[:, None] - channel_window[None, :] // 2, 0, length)
    high = jnp.clip(positions[:, None] + channel_window[None, :] - channel_window[None, :] // 2, 0, length)
    count = (high - low).astype(jnp.float32)
    pool_mixed = (total / count - pool_input.astype(jnp.float32)).astype(bf)
    pool_mixed = pool_mixed.reshape(length, POOL_GROUPS, POOL_GROUP)
    grouped = jnp.einsum('lgc,gcd->lgd', pool_mixed.astype(jnp.float32), w_pool_mix.astype(jnp.float32))
    pool_rows = (grouped.reshape(length, POOL_GROUPS * POOL_GROUP) * pool_scale).astype(bf)
    attn_branch = jnp.dot(attn_rows, w_attn_out, preferred_element_type=jnp.float32)
    pool_branch = jnp.dot(pool_rows, w_pool_out, preferred_element_type=jnp.float32)
    gate_attn = jax.nn.sigmoid(jnp.dot(normed, w_gate_attn, preferred_element_type=jnp.float32))
    gate_pool = jax.nn.sigmoid(jnp.dot(normed, w_gate_pool, preferred_element_type=jnp.float32))
    return (gate_attn * attn_branch + gate_pool * pool_branch).astype(bf)
```

```python
import functools
import math

import jax
import jax.numpy as jnp
from jax import lax
from jax.experimental import pallas as pl
from jax.experimental.pallas import tpu as pltpu
from jax.sharding import PartitionSpec as P

NOPE = 64
ROPE = 32
VALUE_DIM = 64
POOL_GROUPS = 4
POOL_GROUP = 256
LANES = 128
REACH = 2**POOL_GROUPS // 2

eps = 1e-06
theta = 10000.0
f32 = jnp.float32
bf = jnp.bfloat16
MESH = pl.DeviceIdType.MESH


def flip(index, offset):
    bit = 1
    while bit <= offset:
        if offset & bit:
            index = index + bit - 2 * bit * ((index // bit) % 2)
        bit *= 2
    return index


def mm(a, b):
    return jnp.dot(a, b, preferred_element_type=f32)


def kernel(
    n,
    m,
    tokens,
    norm_gain,
    query_gain,
    w_query_up,
    latent_gain,
    w_rotary,
    w_latent_up,
    gain_q,
    gain_k,
    w_pool_mix,
    pool_scale,
    cosine,
    sine,
    h_query_down,
    h_latent_down,
    h_pool_in,
    h_gate_attn,
    h_gate_pool,
    h_attn_out,
    h_pool_out,
    out,
    w_query_down,
    w_latent_down,
    w_pool_in,
    w_gate_attn,
    w_gate_pool,
    w_attn_out,
    w_pool_out,
    tok,
    scaled,
    acc_q,
    acc_l,
    acc_r,
    acc_p,
    acc_ga,
    acc_gp,
    queries,
    latents,
    attn_acc,
    padded,
    attn_rows,
    pool_rows,
    local_sem,
    tok_sem,
    wa_sem,
    wp_sem,
    ar_sem,
    pr_sem,
    halo_sem,
    near_sem,
    far_sem,
    main_sem,
    pair_sem,
    pair_send,
):
    s = lax.axis_index("sp")
    t = lax.axis_index("tp")
    rows, cols = tokens.shape
    pairs = n // 2
    p = s // 2
    y = s % 2
    half = rows // 2
    across = flip(s, 1)
    other = (s + n + 2 * y - 1) % n
    heads = attn_acc.shape[0]
    rank = latents.shape[2] - LANES

    def same_parity(i):
        return ((p + i) % pairs) * 2 + y

    fetches = []
    for i, (far, near) in enumerate(
        (
            (h_latent_down, w_latent_down),
            (h_query_down, w_query_down),
            (h_pool_in, w_pool_in),
            (h_gate_attn, w_gate_attn),
            (h_gate_pool, w_gate_pool),
        )
    ):
        fetch = pltpu.make_async_copy(far, near, local_sem.at[i])
        fetch.start()
        fetches.append(fetch)
    mine = pl.ds(pl.multiple_of(t * cols, cols), cols)
    own_out = []
    for i, (far, near) in enumerate(((h_attn_out, w_attn_out), (h_pool_out, w_pool_out))):
        fetch = pltpu.make_async_copy(far.at[:, mine], near.at[0], local_sem.at[5 + i])
        fetch.start()
        own_out.append(fetch)

    barrier = pltpu.get_barrier_semaphore()
    peers = [(s, flip(t, off)) for off in range(1, m)]
    peers += [(same_parity(i), t) for i in range(1, pairs)]
    peers += [(across, t), (other, t)]
    for peer in peers:
        pl.semaphore_signal(barrier, inc=1, device_id=peer, device_id_type=MESH)
    pl.semaphore_wait(barrier, len(peers))

    def remote(src, dst, send, recv, peer):
        return pltpu.make_async_remote_copy(
            src_ref=src,
            dst_ref=dst,
            send_sem=send,
            recv_sem=recv,
            device_id=peer,
            device_id_type=MESH,
        )

    def push(own, buf, sem, off):
        bit = m // 2
        while bit:
            if off == 0 or bit < (off & -off):
                slot = off ^ bit
                remote(
                    own if off == 0 else buf.at[off],
                    buf.at[slot],
                    sem.at[0, slot],
                    sem.at[1, slot],
                    (s, flip(t, bit)),
                ).start()
            bit //= 2

    def arrive(own, buf, sem, off):
        remote(own, buf.at[off], sem.at[0, off], sem.at[1, off], (s, t)).wait_recv()
        push(own, buf, sem, off)

    def drain(own, buf, sem):
        for slot in range(1, m):
            remote(own, buf.at[slot], sem.at[0, slot], sem.at[1, slot], (s, t)).wait_send()

    push(tokens, tok, tok_sem, 0)

    def share(far, near, sem, off):
        peer = flip(t, off)
        part = pl.ds(pl.multiple_of(peer * cols, cols), cols)
        return remote(far.at[:, part], near.at[off], sem.at[0, off], sem.at[1, off], (s, peer))

    pool_first = [share(h_pool_out, w_pool_out, wp_sem, off) for off in range(1, m)]
    attn_next = [share(h_attn_out, w_attn_out, wa_sem, off) for off in range(1, m)]

    squares = jnp.zeros((rows, 1), f32)

    def ready(off):
        block = flip(t, off)
        raw = (tokens[...] if off == 0 else tok[off]).astype(f32)
        gain = norm_gain[pl.ds(block, 1), :]
        scaled[off] = (raw * gain).astype(bf)
        return jnp.sum(raw * raw, axis=-1, keepdims=True)

    def partial(off, w):
        block = flip(t, off)
        return mm(scaled[off], w[pl.ds(pl.multiple_of(block * cols, cols), cols), :])

    first = list(range(max(m // 2, 1)))
    later = list(range(max(m // 2, 1), m))
    wides = (
        (acc_q, w_query_down),
        (acc_p, w_pool_in),
        (acc_ga, w_gate_attn),
        (acc_gp, w_gate_pool),
    )
    smalls = ((acc_l, w_latent_down), (acc_r, w_rotary))
    for off in first:
        if off:
            arrive(tokens, tok, tok_sem, off)
        squares += ready(off)
        if off == 0:
            for fetch in fetches:
                fetch.wait()
        for acc, w in smalls + wides:
            if off == 0:
                acc[...] = partial(off, w)
            else:
                acc[...] += partial(off, w)
    for off in later:
        arrive(tokens, tok, tok_sem, off)
        if off == later[0]:
            for copy in pool_first + attn_next:
                copy.start()
        squares += ready(off)
        for acc, w in smalls:
            acc[...] += partial(off, w)
    scale = lax.rsqrt(squares / (cols * m) + eps)

    lane = lax.broadcasted_iota(jnp.int32, (rows, LANES), 1)
    low = lane < NOPE

    def rotate(values):
        quarter = ROPE // 2
        partner = jnp.where(
            lane < NOPE + quarter,
            pltpu.roll(values, LANES - quarter, 1),
            pltpu.roll(values, quarter, 1),
        )
        return values * cosine[...] + partner * sine[...]

    def rms(values, gain, width):
        mean = jnp.sum(values * values, axis=-1, keepdims=True) / width
        return values * lax.rsqrt(mean + eps) * gain

    latent = (acc_l[...] * scale).astype(bf).astype(f32)
    latents[0, :, :rank] = rms(latent, latent_gain[...], rank).astype(bf)
    rotary = (acc_r[...] * scale).astype(bf).astype(f32)
    turned = rotate(rotary * gain_k[...])
    latents[0, :, rank:] = jnp.where(low, pltpu.roll(rotary, NOPE, 1), turned).astype(bf)

    core = t % 2
    twin = flip(t, 1)
    my_half = pl.ds(pl.multiple_of(core * half, half), half)
    twin_half = pl.ds(pl.multiple_of((1 - core) * half, half), half)
    near_copy = remote(
        latents.at[0, my_half],
        latents.at[1, my_half],
        near_sem.at[0],
        main_sem.at[1],
        (across, t),
    )
    for i in range(1, pairs):
        slot = 2 * (pairs - i)
        remote(
            latents.at[0, my_half],
            latents.at[slot, my_half],
            near_sem.at[i],
            main_sem.at[slot],
            (same_parity(i), t),
        ).start()
    near_copy.start()

    def main_wait(k):
        remote(
            latents.at[0, my_half],
            latents.at[k, my_half],
            near_sem.at[0],
            main_sem.at[k],
            (s, t),
        ).wait_recv()

    def to_across(k):
        return remote(
            latents.at[k, my_half],
            latents.at[k + 1, my_half],
            far_sem.at[k],
            main_sem.at[k + 1],
            (across, t),
        )

    def to_twin(k):
        return remote(
            latents.at[k, my_half],
            latents.at[k, my_half],
            pair_send.at[k],
            pair_sem.at[k],
            (s, twin),
        )

    def twin_wait(k):
        remote(
            latents.at[k, my_half],
            latents.at[k, twin_half],
            pair_send.at[k],
            pair_sem.at[k],
            (s, twin),
        ).wait_recv()

    def finish(acc, w):
        total = acc[...]
        for off in later:
            total += partial(off, w)
        return total

    pool_input = (finish(acc_p, w_pool_in) * scale).astype(bf).astype(f32)
    padded[pl.ds(REACH, rows), :] = pool_input
    down = remote(
        padded.at[pl.ds(rows, REACH), :],
        padded.at[pl.ds(0, REACH), :],
        halo_sem.at[0],
        halo_sem.at[1],
        ((s + 1) % n, t),
    )
    up = remote(
        padded.at[pl.ds(REACH, REACH), :],
        padded.at[pl.ds(rows + REACH, REACH), :],
        halo_sem.at[2],
        halo_sem.at[3],
        ((s + n - 1) % n, t),
    )
    down.start()
    up.start()

    query_latent = (finish(acc_q, w_query_down) * scale).astype(bf).astype(f32)
    query_normed = rms(query_latent, query_gain[...], query_latent.shape[1]).astype(bf)
    for h in range(heads):
        raw = mm(query_normed, w_query_up[:, h * LANES : (h + 1) * LANES]).astype(bf).astype(f32)
        queries[h] = rotate(rms(raw, gain_q[...], NOPE + ROPE)).astype(bf)
    acc_ga[...] = lax.logistic(finish(acc_ga, w_gate_attn) * scale)
    acc_gp[...] = lax.logistic(finish(acc_gp, w_gate_pool) * scale)

    down.wait_recv()
    up.wait_recv()
    before = padded[pl.ds(0, REACH), :]
    after = padded[pl.ds(rows + REACH, REACH), :]
    padded[pl.ds(0, REACH), :] = before * jnp.where(s > 0, 1.0, 0.0)
    padded[pl.ds(rows + REACH, REACH), :] = after * jnp.where(s < n - 1, 1.0, 0.0)
    groups = w_pool_mix.shape[0]
    position = s * rows + lax.broadcasted_iota(jnp.int32, (rows, 1), 0)
    for j in range(groups):
        group = t * groups + j
        reach = jnp.int32(0)
        for i in range(POOL_GROUPS):
            reach = reach + jnp.where(group == i, 2**i, 0)
        part = slice(j * POOL_GROUP, (j + 1) * POOL_GROUP)
        total = jnp.zeros((rows, POOL_GROUP), f32)
        for shift in range(-REACH, REACH):
            inside = (shift >= -reach) & (shift <= reach - 1)
            total += padded[pl.ds(REACH + shift, rows), part] * jnp.where(inside, 1.0, 0.0)
        start = jnp.maximum(position - reach, 0)
        stop = jnp.minimum(position + reach, rows * n)
        count = (stop - start).astype(f32)
        mixed = (total / count - padded[pl.ds(REACH, rows), part]).astype(bf)
        pool_rows[0, :, part] = (mm(mixed, w_pool_mix[j]) * pool_scale[:, part]).astype(bf)
    push(pool_rows.at[0], pool_rows, pr_sem, 0)

    attn_acc[...] = jnp.zeros_like(attn_acc)
    low_mask = low
    ones = jnp.where(lane == 0, 1.0, 0.0)

    def attend(k):
        latent_block = latents[k, :, :rank]
        turned_block = latents[k, :, rank:].astype(f32)
        shared = jnp.sum(
            jnp.where(low_mask, turned_block * turned_block, 0.0), axis=-1, keepdims=True
        )
        for h in range(heads):
            both = mm(latent_block, w_latent_up[:, h * LANES : (h + 1) * LANES])
            both = both.astype(bf).astype(f32)
            total = jnp.sum(jnp.where(low_mask, both * both, 0.0), axis=-1, keepdims=True)
            level = lax.rsqrt((total + shared) / (NOPE + ROPE) + eps)
            key = (jnp.where(low_mask, both * gain_k[...], turned_block) * level).astype(bf)
            value = jnp.where(low_mask, ones, both).astype(bf)
            scores = lax.dot_general(
                queries[h], key, (((1,), (1,)), ((), ())), preferred_element_type=f32
            )
            attn_acc[h] += mm(jnp.exp2(scores).astype(bf), value)

    def step(i, carry):
        @pl.when(i + 1 < pairs)
        def _():
            main_wait(2 * i + 2)
            to_across(2 * i + 2).start()
            to_twin(2 * i + 2).start()

        @pl.when(i > 0)
        def _():
            twin_wait(2 * i)

        attend(2 * i)
        main_wait(2 * i + 1)
        to_twin(2 * i + 1).start()
        twin_wait(2 * i + 1)
        attend(2 * i + 1)
        return carry

    lax.fori_loop(0, pairs, step, 0)

    for j in range(heads // 2):
        even = attn_acc[2 * j]
        odd = attn_acc[2 * j + 1]
        even = even / even[:, :1]
        odd = odd / odd[:, :1]
        attn_rows[0, :, j * LANES : (j + 1) * LANES] = jnp.where(
            low, pltpu.roll(even, NOPE, 1), odd
        ).astype(bf)
    push(attn_rows.at[0], attn_rows, ar_sem, 0)

    for off in range(1, m):
        arrive(pool_rows.at[0], pool_rows, pr_sem, off)
    for fetch in own_out:
        fetch.wait()
    for copy in pool_first + attn_next:
        copy.wait_recv()
    pool_branch = mm(pool_rows[0], w_pool_out[0])
    for off in range(1, m):
        pool_branch += mm(pool_rows[off], w_pool_out[off])
    acc_gp[...] *= pool_branch
    attn_branch = mm(attn_rows[0], w_attn_out[0])
    for off in range(1, m):
        arrive(attn_rows.at[0], attn_rows, ar_sem, off)
        attn_branch += mm(attn_rows[off], w_attn_out[off])
    out[...] = (acc_ga[...] * attn_branch + acc_gp[...]).astype(bf)

    drain(tokens, tok, tok_sem)
    drain(pool_rows.at[0], pool_rows, pr_sem)
    drain(attn_rows.at[0], attn_rows, ar_sem)
    for copy in pool_first + attn_next:
        copy.wait_send()
    down.wait_send()
    up.wait_send()
    for i in range(pairs):
        remote(
            latents.at[0, my_half], latents.at[0, my_half], near_sem.at[i], main_sem.at[1], (s, t)
        ).wait_send()
    for k in range(1, n):
        to_twin(k).wait_send()
        if k % 2 == 0:
            to_across(k).wait_send()


def body(
    n,
    m,
    tokens,
    norm_gain,
    w_query_down,
    query_gain,
    w_query_up,
    w_latent_down,
    latent_gain,
    w_rotary_key,
    w_latent_up,
    query_head_gain,
    key_head_gain,
    w_pool_in,
    w_pool_mix,
    pool_scale,
    w_attn_out,
    w_pool_out,
    w_gate_attn,
    w_gate_pool,
):
    rows, cols = tokens.shape
    width = NOPE + ROPE
    heads = w_query_up.shape[1] // width
    rank = w_latent_down.shape[1]
    pool = w_pool_in.shape[1]
    spare = LANES - width
    positions = lax.axis_index("sp") * rows + jnp.arange(rows, dtype=jnp.int32)
    freqs = theta ** (-jnp.arange(ROPE // 2, dtype=f32) / (ROPE // 2))
    angles = positions.astype(f32)[:, None] * freqs[None, :]
    cos = jnp.cos(angles)
    sin = jnp.sin(angles)
    cosine = jnp.concatenate(
        [jnp.ones((rows, NOPE), f32), cos, cos, jnp.zeros((rows, spare), f32)], axis=1
    )
    sine = jnp.concatenate(
        [jnp.zeros((rows, NOPE), f32), -sin, sin, jnp.zeros((rows, spare), f32)], axis=1
    )
    query_up = jnp.pad(
        w_query_up.reshape(-1, heads, width), ((0, 0), (0, 0), (0, spare))
    ).reshape(-1, heads * LANES)
    rotary = jnp.pad(w_rotary_key, ((0, 0), (NOPE, spare)))
    gain_q = jnp.pad(query_head_gain * (width**-0.5 * math.log2(math.e)), (0, spare))[None, :]
    gain_k = jnp.pad(key_head_gain, (0, spare))[None, :]
    dma = pltpu.SemaphoreType.DMA
    near = pl.BlockSpec(memory_space=pltpu.VMEM)
    far = pl.BlockSpec(memory_space=pl.ANY)
    return pl.pallas_call(
        functools.partial(kernel, n, m),
        out_shape=jax.ShapeDtypeStruct((rows, cols), bf),
        in_specs=[near] * 13 + [far] * 7,
        out_specs=near,
        scratch_shapes=[
            pltpu.VMEM(w_query_down.shape, bf),
            pltpu.VMEM(w_latent_down.shape, bf),
            pltpu.VMEM(w_pool_in.shape, bf),
            pltpu.VMEM(w_gate_attn.shape, bf),
            pltpu.VMEM(w_gate_pool.shape, bf),
            pltpu.VMEM((m, w_attn_out.shape[0], cols), bf),
            pltpu.VMEM((m, w_pool_out.shape[0], cols), bf),
            pltpu.VMEM((m, rows, cols), bf),
            pltpu.VMEM((m, rows, cols), bf),
            pltpu.VMEM((rows, w_query_down.shape[1]), f32),
            pltpu.VMEM((rows, rank), f32),
            pltpu.VMEM((rows, LANES), f32),
            pltpu.VMEM((rows, pool), f32),
            pltpu.VMEM((rows, cols), f32),
            pltpu.VMEM((rows, cols), f32),
            pltpu.VMEM((heads, rows, LANES), bf),
            pltpu.VMEM((n, rows, rank + LANES), bf),
            pltpu.VMEM((heads, rows, LANES), f32),
            pltpu.VMEM((rows + 2 * REACH, pool), f32),
            pltpu.VMEM((m, rows, heads * VALUE_DIM), bf),
            pltpu.VMEM((m, rows, pool), bf),
            dma((7,)),
            dma((2, m)),
            dma((2, m)),
            dma((2, m)),
            dma((2, m)),
            dma((2, m)),
            dma((4,)),
            dma((n // 2,)),
            dma((n,)),
            dma((n,)),
            dma((n,)),
            dma((n,)),
        ],
        compiler_params=pltpu.CompilerParams(collective_id=0, has_side_effects=True),
    )(
        tokens,
        norm_gain.reshape(m, cols),
        query_gain[None, :],
        query_up,
        latent_gain[None, :],
        rotary,
        w_latent_up,
        gain_q,
        gain_k,
        w_pool_mix,
        pool_scale[None, :],
        cosine,
        sine,
        w_query_down,
        w_latent_down,
        w_pool_in,
        w_gate_attn,
        w_gate_pool,
        w_attn_out,
        w_pool_out,
    )


def solution(mesh):
    placed = (
        P("sp", "tp"),
        P(),
        P(),
        P(),
        P(None, "tp"),
        P(),
        P(),
        P(),
        P(None, "tp"),
        P(),
        P(),
        P(None, "tp"),
        P("tp", None, None),
        P("tp"),
        P("tp", None),
        P("tp", None),
        P(None, "tp"),
        P(None, "tp"),
    )
    held = functools.partial(body, mesh.shape["sp"], mesh.shape["tp"])
    return jax.shard_map(held, mesh=mesh, in_specs=placed, out_specs=P("sp", "tp"), check_vma=False)
```

```python
import functools
import math

import jax
import numpy as np
import jax.numpy as jnp
from jax import lax
from jax.experimental import pallas as pl
from jax.experimental.pallas import tpu as pltpu
from jax.sharding import PartitionSpec as P

NOPE = 64
ROPE = 32
VALUE_DIM = 64
POOL_GROUPS = 4
POOL_GROUP = 256
LANES = 128
REACH = 2**POOL_GROUPS // 2

eps = 1e-06
theta = 10000.0
f32 = jnp.float32
bf = jnp.bfloat16
MESH = pl.DeviceIdType.MESH


def flip(index, offset):
    bit = 1
    while bit <= offset:
        if offset & bit:
            index = index + bit - 2 * bit * ((index // bit) % 2)
        bit *= 2
    return index


def mm(a, b):
    return jnp.dot(a, b, preferred_element_type=f32)


def kernel(
    n,
    m,
    tokens,
    norm_gain,
    query_gain,
    w_query_up,
    latent_gain,
    w_latent_up,
    gain_q,
    gain_k,
    w_pool_mix,
    pool_scale,
    freqs,
    h_rotary,
    h_query_down,
    h_latent_down,
    h_pool_in,
    h_gate_attn,
    h_gate_pool,
    h_attn_out,
    h_pool_out,
    out,
    cosine,
    sine,
    w_rotary,
    w_query_down,
    w_latent_down,
    w_pool_in,
    w_gate_attn,
    w_gate_pool,
    w_attn_out,
    w_pool_out,
    tok,
    scaled,
    acc_q,
    acc_l,
    acc_r,
    acc_p,
    acc_ga,
    acc_gp,
    queries,
    latents,
    attn_acc,
    padded,
    attn_rows,
    pool_rows,
    local_sem,
    tok_sem,
    wa_sem,
    wp_sem,
    ar_sem,
    pr_sem,
    halo_sem,
    near_sem,
    far_sem,
    main_sem,
    pair_sem,
    pair_send,
):
    s = lax.axis_index("sp")
    t = lax.axis_index("tp")
    rows, cols = tokens.shape
    pairs = n // 2
    p = s // 2
    y = s % 2
    half = rows // 2
    across = flip(s, 1)
    other = (s + n + 2 * y - 1) % n
    heads = attn_acc.shape[0]
    rank = latents.shape[2] - LANES

    def gap_of(i):
        odd = i % 2
        return odd * ((i + 1) // 2) + (1 - odd) * ((pairs - i // 2) % pairs)

    def same_parity(i):
        return ((p + i) % pairs) * 2 + y

    fetches = []
    for i, (far, near) in enumerate(
        (
            (h_latent_down, w_latent_down),
            (h_query_down, w_query_down),
            (h_pool_in, w_pool_in),
            (h_gate_attn, w_gate_attn),
            (h_gate_pool, w_gate_pool),
            (h_rotary, w_rotary),
        )
    ):
        fetch = pltpu.make_async_copy(far, near, local_sem.at[i])
        fetch.start()
        fetches.append(fetch)
    mine = pl.ds(pl.multiple_of(t * cols, cols), cols)
    own_out = []
    for i, (far, near) in enumerate(((h_attn_out, w_attn_out), (h_pool_out, w_pool_out))):
        fetch = pltpu.make_async_copy(far.at[:, mine], near.at[0], local_sem.at[6 + i])
        fetch.start()
        own_out.append(fetch)

    barrier = pltpu.get_barrier_semaphore()
    peers = [(s, flip(t, off)) for off in range(1, m)]
    peers += [(same_parity(i), t) for i in range(1, pairs)]
    peers += [(across, t), (other, t)]
    for peer in peers:
        pl.semaphore_signal(barrier, inc=1, device_id=peer, device_id_type=MESH)
    pl.semaphore_wait(barrier, len(peers))

    def remote(src, dst, send, recv, peer):
        return pltpu.make_async_remote_copy(
            src_ref=src,
            dst_ref=dst,
            send_sem=send,
            recv_sem=recv,
            device_id=peer,
            device_id_type=MESH,
        )

    def push(own, buf, sem, off):
        bit = m // 2
        while bit:
            if off == 0 or bit < (off & -off):
                slot = off ^ bit
                remote(
                    own if off == 0 else buf.at[off],
                    buf.at[slot],
                    sem.at[0, slot],
                    sem.at[1, slot],
                    (s, flip(t, bit)),
                ).start()
            bit //= 2

    def arrive(own, buf, sem, off):
        remote(own, buf.at[off], sem.at[0, off], sem.at[1, off], (s, t)).wait_recv()
        push(own, buf, sem, off)

    def drain(own, buf, sem):
        for slot in range(1, m):
            remote(own, buf.at[slot], sem.at[0, slot], sem.at[1, slot], (s, t)).wait_send()

    push(tokens, tok, tok_sem, 0)

    def share(far, near, sem, off):
        peer = flip(t, off)
        part = pl.ds(pl.multiple_of(peer * cols, cols), cols)
        return remote(far.at[:, part], near.at[off], sem.at[0, off], sem.at[1, off], (s, peer))

    pool_first = [share(h_pool_out, w_pool_out, wp_sem, off) for off in range(1, m)]
    attn_next = [share(h_attn_out, w_attn_out, wa_sem, off) for off in range(1, m)]

    squares = jnp.zeros((rows, 1), f32)
    lane = lax.broadcasted_iota(jnp.int32, (rows, LANES), 1)
    low = lane < NOPE
    spare = LANES - NOPE - ROPE
    place = s * rows + lax.broadcasted_iota(jnp.int32, (rows, LANES), 0)
    angles = place.astype(f32) * freqs[...]
    cosine[...] = jnp.cos(angles)
    sine[...] = jnp.sin(angles) * jnp.where(lane < NOPE + ROPE // 2, -1.0, 1.0)
    nothing = jnp.zeros((1, spare), f32)
    gain_q = jnp.concatenate([gain_q[...], nothing], axis=1)
    gain_q = gain_q * ((NOPE + ROPE) ** -0.5 * math.log2(math.e))
    gain_k = jnp.concatenate([gain_k[...], nothing], axis=1)

    def ready(off):
        block = flip(t, off)
        raw = (tokens[...] if off == 0 else tok[off]).astype(f32)
        gain = norm_gain[:, pl.ds(pl.multiple_of(block * cols, cols), cols)]
        scaled[off] = (raw * gain).astype(bf)
        return jnp.sum(raw * raw, axis=-1, keepdims=True)

    def partial(off, w):
        block = flip(t, off)
        return mm(scaled[off], w[pl.ds(pl.multiple_of(block * cols, cols), cols), :])

    first = list(range(max(m // 2, 1)))
    later = list(range(max(m // 2, 1), m))
    wides = (
        (acc_q, w_query_down),
        (acc_p, w_pool_in),
        (acc_ga, w_gate_attn),
        (acc_gp, w_gate_pool),
    )
    smalls = ((acc_l, w_latent_down), (acc_r, w_rotary))
    for off in first:
        if off:
            arrive(tokens, tok, tok_sem, off)
        squares += ready(off)
        if off == 0:
            for fetch in fetches:
                fetch.wait()
        for acc, w in smalls + wides:
            if off == 0:
                acc[...] = partial(off, w)
            else:
                acc[...] += partial(off, w)
    for off in later:
        arrive(tokens, tok, tok_sem, off)
        if off == later[0]:
            for copy in pool_first + attn_next:
                copy.start()
        squares += ready(off)
        for acc, w in smalls:
            acc[...] += partial(off, w)
    scale = lax.rsqrt(squares / (cols * m) + eps)

    def rotate(values):
        quarter = ROPE // 2
        partner = jnp.where(
            lane < NOPE + quarter,
            pltpu.roll(values, LANES - quarter, 1),
            pltpu.roll(values, quarter, 1),
        )
        return values * cosine[...] + partner * sine[...]

    def rms(values, gain, width):
        mean = jnp.sum(values * values, axis=-1, keepdims=True) / width
        return values * lax.rsqrt(mean + eps) * gain

    latent = (acc_l[...] * scale).astype(bf).astype(f32)
    latents[0, :, :rank] = rms(latent, latent_gain[...], rank).astype(bf)
    rotary = (acc_r[...] * scale).astype(bf).astype(f32)
    rotary = jnp.concatenate(
        [jnp.zeros((rows, NOPE), f32), rotary, jnp.zeros((rows, spare), f32)], axis=1
    )
    turned = rotate(rotary * gain_k)
    latents[0, :, rank:] = jnp.where(low, pltpu.roll(rotary, NOPE, 1), turned).astype(bf)

    core = t % 2
    twin = flip(t, 1)
    my_half = pl.ds(pl.multiple_of(core * half, half), half)
    twin_half = pl.ds(pl.multiple_of((1 - core) * half, half), half)
    near_copy = remote(
        latents.at[0, my_half],
        latents.at[1, my_half],
        near_sem.at[0],
        main_sem.at[1],
        (across, t),
    )
    for i in range(1, pairs):
        gap = gap_of(i)
        slot = 2 * gap
        remote(
            latents.at[0, my_half],
            latents.at[slot, my_half],
            near_sem.at[i],
            main_sem.at[slot],
            (same_parity(pairs - gap), t),
        ).start()
    near_copy.start()

    def main_wait(k):
        remote(
            latents.at[0, my_half],
            latents.at[k, my_half],
            near_sem.at[0],
            main_sem.at[k],
            (s, t),
        ).wait_recv()

    def to_across(k):
        return remote(
            latents.at[k, my_half],
            latents.at[k + 1, my_half],
            far_sem.at[k],
            main_sem.at[k + 1],
            (across, t),
        )

    def to_twin(k):
        return remote(
            latents.at[k, my_half],
            latents.at[k, my_half],
            pair_send.at[k],
            pair_sem.at[k],
            (s, twin),
        )

    def twin_wait(k):
        remote(
            latents.at[k, my_half],
            latents.at[k, twin_half],
            pair_send.at[k],
            pair_sem.at[k],
            (s, twin),
        ).wait_recv()

    def finish(acc, w):
        total = acc[...]
        for off in later:
            total += partial(off, w)
        return total

    pool_input = (finish(acc_p, w_pool_in) * scale).astype(bf).astype(f32)
    padded[pl.ds(REACH, rows), :] = pool_input
    down = remote(
        padded.at[pl.ds(rows, REACH), :],
        padded.at[pl.ds(0, REACH), :],
        halo_sem.at[0],
        halo_sem.at[1],
        ((s + 1) % n, t),
    )
    up = remote(
        padded.at[pl.ds(REACH, REACH), :],
        padded.at[pl.ds(rows + REACH, REACH), :],
        halo_sem.at[2],
        halo_sem.at[3],
        ((s + n - 1) % n, t),
    )
    down.start()
    up.start()

    query_latent = (finish(acc_q, w_query_down) * scale).astype(bf).astype(f32)
    query_normed = rms(query_latent, query_gain[...], query_latent.shape[1]).astype(bf)
    query_raw = mm(query_normed, w_query_up[...]).astype(bf).astype(f32)
    for h in range(heads):
        raw = query_raw[:, h * (NOPE + ROPE) : (h + 1) * (NOPE + ROPE)]
        raw = jnp.concatenate([raw, jnp.zeros((rows, spare), f32)], axis=1)
        queries[h] = rotate(rms(raw, gain_q, NOPE + ROPE)).astype(bf)
    acc_ga[...] = lax.logistic(finish(acc_ga, w_gate_attn) * scale)
    acc_gp[...] = lax.logistic(finish(acc_gp, w_gate_pool) * scale)

    down.wait_recv()
    up.wait_recv()
    before = padded[pl.ds(0, REACH), :]
    after = padded[pl.ds(rows + REACH, REACH), :]
    padded[pl.ds(0, REACH), :] = before * jnp.where(s > 0, 1.0, 0.0)
    padded[pl.ds(rows + REACH, REACH), :] = after * jnp.where(s < n - 1, 1.0, 0.0)
    groups = w_pool_mix.shape[0]
    position = s * rows + lax.broadcasted_iota(jnp.int32, (rows, 1), 0)
    for j in range(groups):
        group = t * groups + j
        reach = jnp.int32(0)
        for i in range(POOL_GROUPS):
            reach = reach + jnp.where(group == i, 2**i, 0)
        part = slice(j * POOL_GROUP, (j + 1) * POOL_GROUP)
        total = jnp.zeros((rows, POOL_GROUP), f32)
        for shift in range(-REACH, REACH):
            inside = (shift >= -reach) & (shift <= reach - 1)
            total += padded[pl.ds(REACH + shift, rows), part] * jnp.where(inside, 1.0, 0.0)
        start = jnp.maximum(position - reach, 0)
        stop = jnp.minimum(position + reach, rows * n)
        count = (stop - start).astype(f32)
        mixed = (total / count - padded[pl.ds(REACH, rows), part]).astype(bf)
        pool_rows[0, :, part] = (mm(mixed, w_pool_mix[j]) * pool_scale[:, part]).astype(bf)
    push(pool_rows.at[0], pool_rows, pr_sem, 0)

    attn_acc[...] = jnp.zeros_like(attn_acc)
    low_mask = low
    ones = jnp.where(lane == 0, 1.0, 0.0)

    def attend(k):
        latent_block = latents[k, :, :rank]
        turned_block = latents[k, :, rank:].astype(f32)
        shared = jnp.sum(
            jnp.where(low_mask, turned_block * turned_block, 0.0), axis=-1, keepdims=True
        )
        for h in range(heads):
            both = mm(latent_block, w_latent_up[:, h * LANES : (h + 1) * LANES])
            both = both.astype(bf).astype(f32)
            total = jnp.sum(jnp.where(low_mask, both * both, 0.0), axis=-1, keepdims=True)
            level = lax.rsqrt((total + shared) / (NOPE + ROPE) + eps)
            key = (jnp.where(low_mask, both * gain_k, turned_block) * level).astype(bf)
            value = jnp.where(low_mask, ones, both).astype(bf)
            scores = lax.dot_general(
                queries[h], key, (((1,), (1,)), ((), ())), preferred_element_type=f32
            )
            attn_acc[h] += mm(jnp.exp2(scores).astype(bf), value)

    def step(i, carry):
        now = 2 * gap_of(i)

        @pl.when(i + 1 < pairs)
        def _():
            ahead = 2 * gap_of(i + 1)
            main_wait(ahead)
            to_across(ahead).start()
            to_twin(ahead).start()

        @pl.when(i > 0)
        def _():
            twin_wait(now)

        attend(now)
        main_wait(now + 1)
        to_twin(now + 1).start()
        twin_wait(now + 1)
        attend(now + 1)
        return carry

    lax.fori_loop(0, pairs, step, 0)

    for j in range(heads // 2):
        even = attn_acc[2 * j]
        odd = attn_acc[2 * j + 1]
        even = even / even[:, :1]
        odd = odd / odd[:, :1]
        attn_rows[0, :, j * LANES : (j + 1) * LANES] = jnp.where(
            low, pltpu.roll(even, NOPE, 1), odd
        ).astype(bf)
    push(attn_rows.at[0], attn_rows, ar_sem, 0)

    for off in range(1, m):
        arrive(pool_rows.at[0], pool_rows, pr_sem, off)
    for fetch in own_out:
        fetch.wait()
    for copy in pool_first + attn_next:
        copy.wait_recv()
    pool_branch = mm(pool_rows[0], w_pool_out[0])
    for off in range(1, m):
        pool_branch += mm(pool_rows[off], w_pool_out[off])
    acc_gp[...] *= pool_branch
    attn_branch = mm(attn_rows[0], w_attn_out[0])
    for off in range(1, m):
        arrive(attn_rows.at[0], attn_rows, ar_sem, off)
        attn_branch += mm(attn_rows[off], w_attn_out[off])
    out[...] = (acc_ga[...] * attn_branch + acc_gp[...]).astype(bf)

    drain(tokens, tok, tok_sem)
    drain(pool_rows.at[0], pool_rows, pr_sem)
    drain(attn_rows.at[0], attn_rows, ar_sem)
    for copy in pool_first + attn_next:
        copy.wait_send()
    down.wait_send()
    up.wait_send()
    for i in range(pairs):
        remote(
            latents.at[0, my_half], latents.at[0, my_half], near_sem.at[i], main_sem.at[1], (s, t)
        ).wait_send()
    for k in range(1, n):
        to_twin(k).wait_send()
        if k % 2 == 0:
            to_across(k).wait_send()


def body(
    n,
    m,
    tokens,
    norm_gain,
    w_query_down,
    query_gain,
    w_query_up,
    w_latent_down,
    latent_gain,
    w_rotary_key,
    w_latent_up,
    query_head_gain,
    key_head_gain,
    w_pool_in,
    w_pool_mix,
    pool_scale,
    w_attn_out,
    w_pool_out,
    w_gate_attn,
    w_gate_pool,
):
    rows, cols = tokens.shape
    width = NOPE + ROPE
    heads = w_query_up.shape[1] // width
    rank = w_latent_down.shape[1]
    pool = w_pool_in.shape[1]
    freqs = theta ** (-(np.arange(LANES) % (ROPE // 2)) / (ROPE // 2))
    freqs = np.where(np.arange(LANES) // ROPE == NOPE // ROPE, freqs, 0.0)
    freqs = jnp.asarray(freqs, f32)[None, :]
    dma = pltpu.SemaphoreType.DMA
    near = pl.BlockSpec(memory_space=pltpu.VMEM)
    far = pl.BlockSpec(memory_space=pl.ANY)
    return pl.pallas_call(
        functools.partial(kernel, n, m),
        out_shape=jax.ShapeDtypeStruct((rows, cols), bf),
        in_specs=[near] * 11 + [far] * 8,
        out_specs=near,
        scratch_shapes=[
            pltpu.VMEM((rows, LANES), f32),
            pltpu.VMEM((rows, LANES), f32),
            pltpu.VMEM(w_rotary_key.shape, bf),
            pltpu.VMEM(w_query_down.shape, bf),
            pltpu.VMEM(w_latent_down.shape, bf),
            pltpu.VMEM(w_pool_in.shape, bf),
            pltpu.VMEM(w_gate_attn.shape, bf),
            pltpu.VMEM(w_gate_pool.shape, bf),
            pltpu.VMEM((m, w_attn_out.shape[0], cols), bf),
            pltpu.VMEM((m, w_pool_out.shape[0], cols), bf),
            pltpu.VMEM((m, rows, cols), bf),
            pltpu.VMEM((m, rows, cols), bf),
            pltpu.VMEM((rows, w_query_down.shape[1]), f32),
            pltpu.VMEM((rows, rank), f32),
            pltpu.VMEM((rows, ROPE), f32),
            pltpu.VMEM((rows, pool), f32),
            pltpu.VMEM((rows, cols), f32),
            pltpu.VMEM((rows, cols), f32),
            pltpu.VMEM((heads, rows, LANES), bf),
            pltpu.VMEM((n, rows, rank + LANES), bf),
            pltpu.VMEM((heads, rows, LANES), f32),
            pltpu.VMEM((rows + 2 * REACH, pool), f32),
            pltpu.VMEM((m, rows, heads * VALUE_DIM), bf),
            pltpu.VMEM((m, rows, pool), bf),
            dma((8,)),
            dma((2, m)),
            dma((2, m)),
            dma((2, m)),
            dma((2, m)),
            dma((2, m)),
            dma((4,)),
            dma((n // 2,)),
            dma((n,)),
            dma((n,)),
            dma((n,)),
            dma((n,)),
        ],
        compiler_params=pltpu.CompilerParams(collective_id=0, has_side_effects=True),
    )(
        tokens,
        norm_gain[None, :],
        query_gain[None, :],
        w_query_up,
        latent_gain[None, :],
        w_latent_up,
        query_head_gain[None, :],
        key_head_gain[None, :],
        w_pool_mix,
        pool_scale[None, :],
        freqs,
        w_rotary_key,
        w_query_down,
        w_latent_down,
        w_pool_in,
        w_gate_attn,
        w_gate_pool,
        w_attn_out,
        w_pool_out,
    )


def solution(mesh):
    placed = (
        P("sp", "tp"),
        P(),
        P(),
        P(),
        P(None, "tp"),
        P(),
        P(),
        P(),
        P(None, "tp"),
        P(),
        P(),
        P(None, "tp"),
        P("tp", None, None),
        P("tp"),
        P("tp", None),
        P("tp", None),
        P(None, "tp"),
        P(None, "tp"),
    )
    held = functools.partial(body, mesh.shape["sp"], mesh.shape["tp"])
    return jax.shard_map(held, mesh=mesh, in_specs=placed, out_specs=P("sp", "tp"), check_vma=False)
```
